256 devices in a mesh: sp: 64 (over z, y, core), tp: 4 (over x).
Axes of the slice: x: 4, y: 4, z: 8, core: 2. Of those that a mesh axis runs over, the one named last changes fastest.
Arguments:
- residual: bfloat16 [49152, 2048], P(('sp', 'tp')), may hold values from -6 to 6
- queries: bfloat16 [49152, 1024], P('sp', 'tp'), may hold values from -240 to 240
- keys: bfloat16 [49152, 256], P('sp', 'tp'), may hold values from -6 to 6
- values: bfloat16 [49152, 256], P('sp', 'tp'), may hold values from -18 to 18
- sinks: float32 [16], P('tp'), may hold values from 1 to 6
- out_weight: bfloat16 [1024, 2048], replicated, may hold values from -0.5625 to 0.5625
- norm_gain: float32 [2048], replicated, may hold values from 0.1 to 1.9
- gate_weight: bfloat16 [2048, 5632], P('sp', 'tp'), may hold values from -0.125 to 0.125
- up_weight: bfloat16 [2048, 5632], P('sp', 'tp'), may hold values from -0.125 to 0.125
- down_weight: bfloat16 [5632, 2048], P('tp', 'sp'), may hold values from -0.078125 to 0.078125
Outputs:
- layer_out: bfloat16 [49152, 2048], P(('sp', 'tp'))
The draws below stay inside these ranges and needn't reach their ends.
All inputs are finite; a program needn't handle non-finite values.
Results may differ from the reference program's by a relative error of at most 0.014.
Values may be sent and summed in bfloat16 or wider, within the bound.
A program may use at most 128 MiB of HBM per device.

```python
import jax
import jax.numpy as jnp
from jax import lax

D = 2048
FF = 5632
HEAD = 64
QH = 16
KVH = 4
WINDOW = 128
ATT = 1024
TOKENS = 49152
N_TP = 4


def drawn(key):
    key_query, key_keys = jax.random.split(jax.random.fold_in(key, 7), 2)
    queries = jnp.clip(jax.random.normal(key_query, (TOKENS, QH * HEAD), jnp.float32), -6.0, 6.0)
    keyset = jnp.clip(jax.random.normal(key_keys, (TOKENS, KVH * HEAD), jnp.float32), -6.0, 6.0)
    return (queries, keyset)


def draw_queries(key, part):
    return drawn(key)[0].astype(jnp.bfloat16)


def draw_keys(key, part):
    return drawn(key)[1].astype(jnp.bfloat16)


def steps_of(rng, extent, shards, least, largest):
    def one(axis_at, shards_of):
        draws = jax.random.uniform(jax.random.fold_in(jax.random.fold_in(rng, 6), axis_at), (shards_of,), jnp.float32, least / len(shards), largest / len(shards))
        return jnp.repeat(jnp.exp(draws), extent[axis_at] // shards_of).reshape((-1,) + (1,) * (len(extent) - axis_at - 1))

    loudness = one(*shards[0])
    for cut in shards[1:]:
        loudness = loudness * one(*cut)
    return loudness


def gaussian(own_key, extent, spread, bound, shards=(), dtype=jnp.bfloat16):
    values = spread * jax.random.normal(own_key, extent, jnp.float32)
    if shards:
        values = values * steps_of(own_key, extent, shards, -0.22, 0.18)
    return jnp.clip(values, -bound, bound).astype(dtype)


def setup_inputs(seed: int = 0) -> dict:
    splits = jax.random.split(jax.random.key(seed), 11)
    residual = gaussian(splits[0], (TOKENS, D), 1.0, 6.0, ((0, 256),))
    queries = draw_queries(jax.random.fold_in(splits[10], 71), 0)
    keys = draw_keys(jax.random.fold_in(splits[10], 71), 0)
    values = gaussian(splits[3], (TOKENS, KVH * HEAD), 3.0, 18.0, ((0, 64), (1, 4)))
    sinks = jnp.clip(1.0 + 5.0 * jax.random.uniform(splits[4], (QH,), jnp.float32) ** steps_of(splits[4], (QH,), ((0, 4),), -0.2, 0.2), 1.0, 6.0)
    out_weight = gaussian(splits[5], (ATT, D), (3.0 / ATT ** 0.5), 0.5625)
    norm_gain = jnp.clip(1.0 + 0.18 * jax.random.normal(splits[6], (D,), jnp.float32), 0.1, 1.9)
    gate_weight = gaussian(splits[7], (D, FF), D ** -0.5, 0.125, ((0, 64), (1, 4)))
    up_weight = gaussian(splits[8], (D, FF), D ** -0.5, 0.125, ((0, 64), (1, 4)))
    down_weight = gaussian(splits[9], (FF, D), FF ** -0.5, 0.078125, ((0, 4), (1, 64)))
    return {"residual": residual, "queries": queries, "keys": keys, "values": values, "sinks": sinks, "out_weight": out_weight, "norm_gain": norm_gain, "gate_weight": gate_weight, "up_weight": up_weight, "down_weight": down_weight}


def attend(queries, keys_ext, values_ext, sinks, block_base):
    rows = queries.shape[0]
    nblk = rows // WINDOW
    qheads = sinks.shape[0]
    kheads = keys_ext.shape[1] // HEAD
    group = qheads // kheads
    qblock = queries.reshape(nblk, WINDOW, kheads, group, HEAD).astype(jnp.float32)

    def band(arr):
        first = arr[:rows].reshape(nblk, WINDOW, kheads, HEAD)
        second = arr[WINDOW:].reshape(nblk, WINDOW, kheads, HEAD)
        return jnp.concatenate([first, second], axis=1).astype(jnp.float32)
    kband = band(keys_ext)
    vband = band(values_ext)
    score = jnp.einsum('nqhgd,nkhd->nhgqk', qblock, kband) * HEAD ** (-0.5)
    qidx = jnp.arange(WINDOW)[:, None]
    kidx = jnp.arange(2 * WINDOW)[None, :]
    rel = qidx + WINDOW - kidx
    valid = (rel >= 0) & (rel < WINDOW)
    blocks = block_base + jnp.arange(nblk)
    valid = valid[None] & ((blocks > 0)[:, None, None] | (kidx >= WINDOW)[None])
    score = jnp.where(valid[:, None, None], score, -jnp.inf)
    sink = sinks.astype(jnp.float32).reshape(kheads, group)[None, :, :, None]
    top = jnp.maximum(lax.optimization_barrier(jnp.max(score, axis=-1)), sink)
    expd = jnp.exp(score - top[..., None])
    denom = lax.optimization_barrier(jnp.sum(expd, axis=-1)) + jnp.exp(sink - top)
    weights = (expd / denom[..., None]).astype(jnp.bfloat16)
    result = jnp.einsum('nhgqk,nkhd->nqhgd', weights.astype(jnp.float32), vband)
    return result.reshape(rows, qheads * HEAD).astype(jnp.bfloat16)

def reference(residual, queries, keys, values, sinks, out_weight, norm_gain, gate_weight, up_weight, down_weight):
    padding = jnp.zeros((WINDOW, keys.shape[1]), jnp.bfloat16)
    keys_ext = jnp.concatenate([padding, keys], axis=0)
    values_ext = jnp.concatenate([padding, values], axis=0)
    attention = attend(queries, keys_ext, values_ext, sinks, 0)
    proj = jnp.dot(attention, out_weight, preferred_element_type=jnp.float32)
    mixed = (residual.astype(jnp.float32) + proj).astype(jnp.bfloat16)
    mixf = mixed.astype(jnp.float32)
    normed = (mixf * lax.rsqrt(lax.optimization_barrier(jnp.mean(mixf * mixf, axis=-1, keepdims=True)) + 1e-06) * norm_gain).astype(jnp.bfloat16)
    gate = jnp.dot(normed, gate_weight, preferred_element_type=jnp.float32)
    upper = jnp.dot(normed, up_weight, preferred_element_type=jnp.float32)
    hidden = (jax.nn.silu(gate) * upper).astype(jnp.bfloat16)
    share = FF // N_TP
    ffn = jnp.zeros((hidden.shape[0], D), jnp.float32)
    for index in range(N_TP):
        part_sum = jnp.dot(hidden[:, index * share:(index + 1) * share], down_weight[index * share:(index + 1) * share], preferred_element_type=jnp.float32)
        ffn = ffn + lax.optimization_barrier(part_sum.astype(jnp.bfloat16)).astype(jnp.float32)
    return (mixed.astype(jnp.float32) + ffn).astype(jnp.bfloat16)
```

```python
import functools

import jax
import jax.numpy as jnp
from jax import lax
from jax.experimental import pallas as pl
from jax.experimental.pallas import tpu as pltpu
from jax.sharding import PartitionSpec as P

MESH = pl.DeviceIdType.MESH
BF16, F32 = jnp.bfloat16, jnp.float32
HEAD = 64
WINDOW = 128
NZ, NY, NC, NX = 8, 4, 2, 4
ROWS = 768
MINE = 192
D, FFD = 2048, 1408
GA = 4
DA = 640
NT = (((1,), (1,)), ((), ()))
LABELS = (0, -1, 1, -2, 2, -3, 3, -4)
PER = 57


def kernel(
    res_h, q_h, k_h, v_h, sink_s, wo_h, gain_h, g_h, u_h, d_h, out_h,
    gu, dt, xs, hid, ao, at, wo, res, mix, qv, kx, vx, gain, draw,
    sa, sm, sp_, ra, rfm, rfp, own, outv,
    load_sem, out_sem, gs, gr, ds_, dr, as_, ar, xsend, xrecv, rsend, rrecv, hsem,
):
    sp = lax.axis_index("sp")
    x = lax.axis_index("tp")
    z, y, c = sp // (NY * NC), (sp // NC) % NY, sp % NC
    s = 1 - 2 * c

    def spidx(zz, yy, cc):
        return (zz * NY + yy) * NC + cc

    def zat(k):
        return (z + k * s + NZ) % NZ

    def yat(k):
        return (y + k * s + NY) % NY

    def xat(k):
        return (x + k * s + NX) % NX

    to_yp = {"sp": spidx(z, yat(1), c)}
    to_ym = {"sp": spidx(z, yat(-1), c)}
    to_zp = {"sp": spidx(zat(1), y, c)}
    to_zm = {"sp": spidx(zat(-1), y, c)}
    to_core = {"sp": spidx(z, y, 1 - c)}
    to_xp = {"tp": xat(1)}
    to_xm = {"tp": xat(-1)}
    nsp = NZ * NY * NC
    to_next = {"sp": (sp + 1) % nsp}
    to_prev = {"sp": (sp + nsp - 1) % nsp}

    def load(src, dst, i):
        pltpu.make_async_copy(src, dst, load_sem.at[i]).start()

    def loaded(dst, i):
        pltpu.make_async_copy(dst, dst, load_sem.at[i]).wait()

    for n in range(11):
        load(g_h.at[:, pl.ds(128 * n, 128)], gu.at[n, z, y, c, :, pl.ds(0, 128)], 0)
        load(u_h.at[:, pl.ds(128 * n, 128)], gu.at[n, z, y, c, :, pl.ds(128, 128)], 0)
    load(k_h, kx.at[pl.ds(WINDOW, ROWS)], 1)
    load(v_h, vx.at[pl.ds(WINDOW, ROWS)], 2)
    load(q_h, qv, 3)
    load(d_h, draw, 4)
    for n in range(8):
        load(wo_h.at[:, pl.ds(256 * n, 256)], wo.at[n], 5)
        load(res_h.at[:, pl.ds(256 * n, 256)], res.at[n], 6)
    load(gain_h, gain, 7)

    barrier = pltpu.get_barrier_semaphore()
    peers = [to_yp, to_ym, to_zp, to_zm, to_core, to_next, to_prev]
    peers += [{"tp": (x + j) % NX} for j in (1, 2, 3)]
    for peer in peers:
        pl.semaphore_signal(barrier, inc=1, device_id=peer, device_id_type=MESH)
    pl.semaphore_wait(barrier, len(peers))

    def remote(src, dst, send, recv, to):
        return pltpu.make_async_remote_copy(
            src_ref=src, dst_ref=dst, send_sem=send, recv_sem=recv, device_id=to, device_id_type=MESH
        )

    ALL = slice(None)

    def gu_at(part, zz, yy, cc):
        tiles = pl.ds(0, GA) if part == "a" else pl.ds(GA, 11 - GA)
        return gu.at[tiles, zz, yy, cc]

    def dt_at(part, zz, yy, cc):
        lanes = pl.ds(0, DA) if part == "a" else pl.ds(DA, FFD - DA)
        return dt.at[zz, yy, cc, :, lanes]

    def stream(view, send_sem, recv_sem):
        slots = {}

        def slot(key):
            return slots.setdefault(key, len(slots))

        sent = []

        def send(key, part, zz, yy, to):
            i = slot(key)
            copy = remote(
                view(part, zz, yy, c), view(part, zz, yy, c), send_sem.at[i], recv_sem.at[i], to
            )
            copy.start()
            sent.append(copy)

        def recv(key, part, zz, yy, cc=None):
            i = slot(key)
            ref = view(part, zz, yy, c if cc is None else cc)
            remote(ref, ref, send_sem.at[i], recv_sem.at[i], to_core).wait_recv()

        def start():
            send("ay-1", "a", z, y, to_yp)
            send("ay+1", "a", z, y, to_ym)
            send("bz-1", "b", z, y, to_zp)
            send("bz+1", "b", z, y, to_zm)
            by_out(0)

        def by_out(k):
            send(f"by-1,{k}", "b", zat(k), y, to_yp)
            send(f"by+1,{k}", "b", zat(k), y, to_ym)

        def a_y1():
            recv("ay-1", "a", z, yat(-1))
            send("ay-2", "a", z, yat(-1), to_yp)
            recv("ay+1", "a", z, yat(1))

        def a_y2():
            recv("ay-2", "a", z, yat(-2))
            send("az-1", "a", z, ALL, to_zp)
            send("az+1", "a", z, ALL, to_zm)
            send("ad0", "a", z, ALL, to_core)

        def a_z(k):
            recv(f"az{k:+d}", "a", zat(k), ALL)
            if -4 < k < 0:
                send(f"az{k - 1:+d}", "a", zat(k), ALL, to_zp)
            if 0 < k < 3:
                send(f"az{k + 1:+d}", "a", zat(k), ALL, to_zm)
            send(f"ad{k}", "a", zat(k), ALL, to_core)

        def b_z(k):
            recv(f"bz{k:+d}", "b", zat(k), y)
            if -4 < k < 0:
                send(f"bz{k - 1:+d}", "b", zat(k), y, to_zp)
            if 0 < k < 3:
                send(f"bz{k + 1:+d}", "b", zat(k), y, to_zm)
            by_out(k)

        def b_y1(k):
            recv(f"by-1,{k}", "b", zat(k), yat(-1))
            send(f"by-2,{k}", "b", zat(k), yat(-1), to_yp)
            recv(f"by+1,{k}", "b", zat(k), yat(1))

        def b_y2(k):
            recv(f"by-2,{k}", "b", zat(k), yat(-2))
            send(f"bd{k}", "b", zat(k), ALL, to_core)

        def partner(part, k):
            zz = (z - k * s + NZ) % NZ
            recv(f"{part}d{k}", part, zz, ALL, 1 - c)

        f = functools.partial
        events = [
            f(a_y1),
            f(b_z, -1), f(b_z, 1),
            f(a_y2),
            f(b_y1, 0),
            f(b_z, -2), f(b_z, 2),
            f(b_y2, 0),
            f(a_z, -1), f(a_z, 1),
            f(b_y1, -1), f(b_y1, 1),
            f(b_z, -3), f(b_z, 3),
            f(b_y2, -1), f(b_y2, 1),
            f(b_z, -4),
            f(a_z, -2), f(a_z, 2),
            f(b_y1, -2), f(b_y1, 2),
            f(b_y2, -2), f(b_y2, 2),
            f(a_z, -3), f(a_z, 3),
            f(b_y1, -3), f(b_y1, 3),
            f(b_y2, -3), f(b_y2, 3),
            f(a_z, -4),
            f(b_y1, -4), f(b_y2, -4),
        ]
        last = [f(partner, p, k) for k in LABELS for p in "ab"]
        return start, events, last, sent

    gstart, gevents, glast, gsent = stream(gu_at, gs, gr)
    dstart, devents, dlast, dsent = stream(dt_at, ds_, dr)

    loaded(gu.at[:, z, y, c], 0)
    gstart()

    loaded(kx.at[pl.ds(WINDOW, ROWS)], 1)
    loaded(vx.at[pl.ds(WINDOW, ROWS)], 2)
    halo = []
    for i, buf in enumerate((kx, vx)):
        copy = remote(
            buf.at[pl.ds(ROWS, WINDOW)], buf.at[pl.ds(0, WINDOW)], hsem.at[i], hsem.at[2 + i], to_next
        )
        copy.start()
        halo.append(copy)

    loaded(qv, 3)
    sink = jnp.concatenate([jnp.full((WINDOW, 1), sink_s[h], F32) for h in range(4)], axis=0)
    qi = lax.broadcasted_iota(jnp.int32, (4 * WINDOW, 2 * WINDOW), 0) % WINDOW
    ki = lax.broadcasted_iota(jnp.int32, (4 * WINDOW, 2 * WINDOW), 1)
    rel = qi + WINDOW - ki
    inside = (rel >= 0) & (rel < WINDOW)

    def attend(b, valid):
        q = qv[pl.ds(pl.multiple_of(b * WINDOW, WINDOW), WINDOW), :]
        q = jnp.concatenate([q[:, h * HEAD : (h + 1) * HEAD] for h in range(4)], axis=0)
        band = pl.ds(pl.multiple_of(b * WINDOW, WINDOW), 2 * WINDOW)
        score = lax.dot_general(q, kx[band, :], NT, preferred_element_type=F32) * HEAD ** (-0.5)
        score = jnp.where(valid, score, -1e30)
        top = jnp.maximum(jnp.max(score, axis=-1, keepdims=True), sink)
        expd = jnp.exp(score - top)
        denom = jnp.sum(expd, axis=-1, keepdims=True) + jnp.exp(sink - top)
        weights = (expd * (1.0 / denom)).astype(BF16)
        o = jnp.dot(weights, vx[band, :], preferred_element_type=F32).astype(BF16)
        o = jnp.concatenate([o[h * WINDOW : (h + 1) * WINDOW] for h in range(4)], axis=1)
        ao[pl.ds(pl.multiple_of(b * WINDOW, WINDOW), WINDOW), :] = o

    @pl.loop(1, ROWS // WINDOW)
    def _(b):
        attend(b, inside)

    for copy in halo:
        copy.wait_recv()
    attend(0, inside & ((ki >= WINDOW) | (sp > 0)))

    asent = []
    for j in (1, 2, 3):
        to = (x + j) % NX
        copy = remote(
            ao.at[pl.ds(pl.multiple_of(to * MINE, MINE), MINE)], at.at[x], as_.at[j], ar.at[j], {"tp": to}
        )
        copy.start()
        asent.append(copy)
    at[x] = ao[pl.ds(pl.multiple_of(x * MINE, MINE), MINE), :]

    gi = iter(gevents)
    di = iter(devents)

    def run(it, count):
        for _ in range(count):
            next(it)()

    run(gi, 3)

    for j in (1, 2, 3):
        src = (x + NX - j) % NX
        remote(at.at[src], at.at[src], as_.at[j], ar.at[j], to_xp).wait_recv()

    loaded(wo, 5)
    loaded(res, 6)
    loaded(gain, 7)
    square = jnp.zeros((MINE, 1), F32)
    for n in range(8):
        acc = res[n].astype(F32)
        proj = jnp.zeros((MINE, 256), F32)
        for i in range(NX):
            proj += jnp.dot(at[i], wo[n, 256 * i : 256 * (i + 1), :], preferred_element_type=F32)
        m = (acc + proj).astype(BF16)
        mix[n] = m
        mf = m.astype(F32)
        square += jnp.sum(mf * mf, axis=-1, keepdims=True)
    scale = lax.rsqrt(square * (1.0 / D) + 1e-06)
    for n in range(8):
        mf = mix[n].astype(F32)
        xs[x, :, 256 * n : 256 * (n + 1)] = (
            mf * scale * gain[:, 256 * n : 256 * (n + 1)]
        ).astype(BF16)

    xsent = []

    def xsend_piece(kind, j, who, to):
        piece = xs.at[who, pl.ds(48 * j, 48)]
        copy = remote(piece, piece, xsend.at[4 * kind + j], xrecv.at[4 * kind + j], to)
        copy.start()
        xsent.append(copy)

    def xrecv_piece(kind, j, who):
        piece = xs.at[who, pl.ds(48 * j, 48)]
        remote(piece, piece, xsend.at[4 * kind + j], xrecv.at[4 * kind + j], to_xp).wait_recv()

    for j in range(4):
        xsend_piece(0, j, x, to_xp)
        xsend_piece(1, j, x, to_xm)

    loaded(draw, 4)
    eye = (
        lax.broadcasted_iota(jnp.int32, (32, 32), 0) == lax.broadcasted_iota(jnp.int32, (32, 32), 1)
    ).astype(BF16)
    dt[z, y, c] = lax.dot_general(eye, draw[...], NT, preferred_element_type=F32).astype(BF16)

    for j in range(4):
        run(gi, 5)
        xrecv_piece(0, j, xat(-1))
        xsend_piece(2, j, xat(-1), to_xp)
    run(gi, 4)
    dstart()
    run(gi, len(gevents) - 27)
    run(di, 3)
    for ev in glast:
        ev()

    def hidden(who, lo, hi):
        @pl.loop(lo, hi)
        def _(n):
            w = gu[n].reshape(D, 256)
            both = jnp.dot(xs[who], w, preferred_element_type=F32)
            gate, up = both[:, :128], both[:, 128:]
            hid[who, :, pl.ds(pl.multiple_of(n * 128, 128), 128)] = (
                gate / (1.0 + jnp.exp(-gate)) * up
            ).astype(BF16)

    for j in range(4):
        xrecv_piece(1, j, xat(1))
    who_list = (x, xat(-1), xat(1), xat(2))
    for w, who in enumerate(who_list):
        if w == 3:
            for j in range(4):
                xrecv_piece(2, j, xat(2))
        hidden(who, 0, 4)
        run(di, 2)
        hidden(who, 4, 8)
        run(di, 2)
        hidden(who, 8, 11)
        run(di, 3)
    run(di, len(devents) - 31)
    for ev in dlast:
        ev()

    def partial(who, n):
        w = dt[n].reshape(256, FFD)
        return lax.dot_general(hid[who], w, NT, preferred_element_type=F32)

    def rs(buf, dst, kind, j, to):
        return remote(
            buf.at[pl.ds(2 * j, 2)], dst.at[pl.ds(2 * j, 2)],
            rsend.at[4 * kind + j], rrecv.at[4 * kind + j], to,
        )

    @pl.loop(0, 4)
    def _(j):
        for i in range(2):
            sa[2 * j + i] = partial(xat(2), 2 * j + i).astype(BF16)
        rs(sa, ra, 0, j, to_xp).start()
        for i in range(2):
            sm[2 * j + i] = partial(xat(-1), 2 * j + i).astype(BF16)
        rs(sm, rfp, 1, j, to_xm).start()

    @pl.loop(0, 8)
    def _(n):
        own[n] = partial(x, n) + mix[n].astype(F32)

    @pl.loop(0, 4)
    def _(j):
        rs(sa, ra, 0, j, to_xp).wait_recv()
        for i in range(2):
            n = 2 * j + i
            sp_[n] = (partial(xat(1), n) + ra[n].astype(F32)).astype(BF16)
        rs(sp_, rfm, 2, j, to_xp).start()

    def out_copy(n):
        return pltpu.make_async_copy(
            outv.at[n], out_h.at[:, pl.ds(pl.multiple_of(n * 256, 256), 256)], out_sem.at[n]
        )

    @pl.loop(0, 4)
    def _(j):
        rs(sm, rfp, 1, j, to_xm).wait_recv()
        rs(sp_, rfm, 2, j, to_xp).wait_recv()
        for i in range(2):
            n = 2 * j + i
            outv[n] = (own[n] + rfp[n].astype(F32) + rfm[n].astype(F32)).astype(BF16)
            out_copy(n).start()

    for copy in halo + asent + xsent + gsent + dsent:
        copy.wait_send()

    @pl.loop(0, 4)
    def _(j):
        rs(sa, ra, 0, j, to_xp).wait_send()
        rs(sm, rfp, 1, j, to_xm).wait_send()
        rs(sp_, rfm, 2, j, to_xp).wait_send()

    @pl.loop(0, 8)
    def _(n):
        out_copy(n).wait()


def shards(residual, queries, keys, values, sinks, out_weight, norm_gain, gate, up, down):
    vmem = pltpu.VMEM
    dma = pltpu.SemaphoreType.DMA
    anyspec = pl.BlockSpec(memory_space=pl.ANY)
    smem = pl.BlockSpec(memory_space=pltpu.SMEM)
    return pl.pallas_call(
        kernel,
        out_shape=jax.ShapeDtypeStruct((MINE, D), BF16),
        in_specs=[anyspec] * 4 + [smem] + [anyspec] * 5,
        out_specs=anyspec,
        scratch_shapes=[
            vmem((11, NZ, NY, NC, 32, 256), BF16),
            vmem((NZ, NY, NC, 32, FFD), BF16),
            vmem((NX, MINE, D), BF16),
            vmem((NX, MINE, FFD), BF16),
            vmem((ROWS, 256), BF16),
            vmem((NX, MINE, 256), BF16),
            vmem((8, 1024, 256), BF16),
            vmem((8, MINE, 256), BF16),
            vmem((8, MINE, 256), BF16),
            vmem((ROWS, 256), BF16),
            vmem((ROWS + WINDOW, HEAD), BF16),
            vmem((ROWS + WINDOW, HEAD), BF16),
            vmem((1, D), F32),
            vmem((FFD, 32), BF16),
        ]
        + [vmem((8, MINE, 256), BF16)] * 6
        + [
            vmem((8, MINE, 256), F32),
            vmem((8, MINE, 256), BF16),
            dma((8,)),
            dma((8,)),
            dma((PER,)), dma((PER,)), dma((PER,)), dma((PER,)),
            dma((4,)), dma((4,)),
            dma((12,)), dma((12,)),
            dma((12,)), dma((12,)),
            dma((4,)),
        ],
        compiler_params=pltpu.CompilerParams(
            collective_id=0, has_side_effects=True, vmem_limit_bytes=62 * 1024 * 1024
        ),
    )(residual, queries, keys, values, sinks, out_weight, norm_gain.reshape(1, D), gate, up, down)


def solution(mesh):
    placed = (
        P(("sp", "tp"), None),
        P("sp", "tp"),
        P("sp", "tp"),
        P("sp", "tp"),
        P("tp"),
        P(),
        P(),
        P("sp", "tp"),
        P("sp", "tp"),
        P("tp", "sp"),
    )
    return jax.shard_map(
        shards, mesh=mesh, in_specs=placed, out_specs=P(("sp", "tp"), None), check_vma=False
    )
```

```python
import jax
import jax.numpy as jnp
from jax import lax
from jax.experimental import pallas as pl
from jax.experimental.pallas import tpu as pltpu
from jax.sharding import PartitionSpec as P

MESH = pl.DeviceIdType.MESH
BF16, F32 = jnp.bfloat16, jnp.float32
HEAD = 64
WINDOW = 128
NZ, NY, NC, NX = 8, 4, 2, 4
ROWS = 768
MINE = 192
D, FFD = 2048, 1408
GA = 4
DA = 640
NT = (((1,), (1,)), ((), ()))
LABELS = (0, -1, 1, -2, 2, -3, 3, -4)
PER = 57
EARLY = (1, 2, 3)

ORDER = (
    "gstart", "halo", "gbo0", "at4", "at5", "at0", "a2a", "gay-1", "gay+1", "gbz-1", "gbz+1", "gbo-1", "gbo1",
    "gby-1,0", "gby+1,0", "gay-2", "gao", "gad0", "oproj", "gbz-2", "gbz+2", "gbo-2", "gbo2", "gby-1,-1",
    "gby+1,-1", "gby-1,1", "gby+1,1", "gby-2,0", "gby+1,-2", "gaz-1", "dstart", "gaz+1", "gbd0", "xf0", "xm0",
    "gad-1", "gby-1,-2", "gad1", "gby+1,2", "gbz-3", "gbo-3", "gbz+3", "gbo3", "day+1", "gby-1,2", "dbz+1",
    "gby-2,-1", "xf1", "xm1", "gbd-1", "gby-2,1", "gby+1,-3", "day-1", "gaz-2", "gbd1", "dbz-1", "gaz+2", "xf2",
    "gad-2", "xm2", "gby+1,3", "gby-2,-2", "dbz+2", "gad2", "gbz-4", "gbo-4", "gby-1,-3", "gbd-2", "gby-1,3", "xf3",
    "xm3", "gby-2,2", "day-2", "gaz-3", "gby+1,-4", "xa0", "gbd2", "gby-1,-4", "dbo0", "dbo-1", "dbz-2", "dbo1",
    "dbo-2", "dbo2", "gaz+3", "dao", "gad-3", "dbz+3", "dbo3", "gby-2,-3", "xa1", "gad3", "dad0", "gby-2,3",
    "gbd-3", "xa2", "dby+1,0", "gbd3", "dby+1,-1", "gby-2,-4", "xa3", "dby+1,1", "gaz-4", "dby-1,0", "daz+1",
    "dbz-3", "dbo-3", "dby+1,-2", "gbd-4", "dby-1,-1", "gad-4", "h1,0,1", "dby+1,2", "dby-1,1", "dad1", "h1,1,2",
    "daz-1", "h1,2,3", "dby-1,-2", "dby+1,3", "h1,3,4", "dby-1,2", "dbz-4", "dbo-4", "dby+1,-3", "dad-1", "h1,4,5",
    "dby-1,3", "h1,5,6", "daz+2", "dby-1,-3", "dby-2,0", "h1,6,7", "dby-2,-1", "h1,7,8", "daz-2", "dby-2,1", "dad2",
    "h1,8,9", "dbd0", "dby+1,-4", "dby-2,-2", "dbd-1", "h1,9,10", "dby-2,2", "dad-2", "h1,10,11", "dby-1,-4",
    "dbd1", "pa0", "dby-2,-3", "dby-2,3", "dbd-2", "dbd2", "pa1", "daz+3", "h0,0,1", "daz-3", "dbd-3", "h0,1,2",
    "dby-2,-4", "dbd3", "h0,2,3", "dad3", "h0,3,4", "dad-3", "pa2", "dbd-4", "h0,4,5", "sp0", "h0,5,7", "daz-4",
    "h0,7,8", "sp1", "h0,8,10", "dad-4", "h0,10,11", "sp2", "pa3", "pm0", "pm1", "pm2", "pm3", "fin0", "sp3",
    "fin1", "fin2", "fin3",
)


def kernel(
    res_h, q_h, k_h, v_h, sink_s, wo_h, gain_h, g_h, u_h, d_h, out_h,
    gu, dt, xs, hid, ao, at, wo, res, mix, qv, kx, vx, gain, bias,
    sa, sm, sp_, ra, rfm, rfp, own, part, outv,
    load_sem, out_sem, gs, gr, ds_, dr, as_, ar, xsend, xrecv, rsend, rrecv, hsem,
):
    sp = lax.axis_index("sp")
    x = lax.axis_index("tp")
    z, y, c = sp // (NY * NC), (sp // NC) % NY, sp % NC
    s = 1 - 2 * c

    def spidx(zz, yy, cc):
        return (zz * NY + yy) * NC + cc

    def zat(k):
        return (z + k * s + NZ) % NZ

    def yat(k):
        return (y + k * s + NY) % NY

    def xat(k):
        return (x + k * s + NX) % NX

    to_yp = {"sp": spidx(z, yat(1), c)}
    to_ym = {"sp": spidx(z, yat(-1), c)}
    to_zp = {"sp": spidx(zat(1), y, c)}
    to_zm = {"sp": spidx(zat(-1), y, c)}
    to_core = {"sp": spidx(z, y, 1 - c)}
    to_xp = {"tp": xat(1)}
    to_xm = {"tp": xat(-1)}
    nsp = NZ * NY * NC
    none = sp // nsp
    to_next = {"sp": (sp + 1) % nsp}
    to_prev = {"sp": (sp + nsp - 1) % nsp}

    barrier = pltpu.get_barrier_semaphore()
    peers = [to_yp, to_ym, to_zp, to_zm, to_core, to_next, to_prev]
    peers += [{"tp": (x + j) % NX} for j in (1, 2, 3)]
    for peer in peers:
        pl.semaphore_signal(barrier, inc=1, device_id=peer, device_id_type=MESH)

    def load(src, dst, i):
        pltpu.make_async_copy(src, dst, load_sem.at[i]).start()

    def loaded(dst, i):
        pltpu.make_async_copy(dst, dst, load_sem.at[i]).wait()

    load(q_h, qv, 3)
    for half in range(2):
        load(k_h, kx.at[pl.ds(half * HEAD, HEAD), pl.ds(WINDOW, ROWS)], 1)
        load(v_h, vx.at[pl.ds(half * HEAD, HEAD), pl.ds(WINDOW, ROWS)], 2)
    for n in range(11):
        load(g_h.at[:, pl.ds(128 * n, 128)], gu.at[n, z, y, c, :, pl.ds(0, 128)], 0)
        load(u_h.at[:, pl.ds(128 * n, 128)], gu.at[n, z, y, c, :, pl.ds(128, 128)], 0)
    load(d_h, dt.at[z, y, c], 4)
    for n in range(8):
        load(wo_h.at[:, pl.ds(256 * n, 256)], wo.at[n], 5)
        load(res_h.at[:, pl.ds(256 * n, 256)], res.at[n], 6)
    load(gain_h, gain, 7)

    def remote(src, dst, send, recv, to):
        return pltpu.make_async_remote_copy(
            src_ref=src, dst_ref=dst, send_sem=send, recv_sem=recv, device_id=to, device_id_type=MESH
        )

    steps = {}
    sent = []

    def begin(copy):
        copy.start()
        sent.append(copy)

    ALL = slice(None)

    def gu_at(half, zz, yy, cc):
        tiles = pl.ds(0, GA) if half == "a" else pl.ds(GA, 11 - GA)
        return gu.at[tiles, zz, yy, cc]

    def dt_at(half, zz, yy, cc):
        lanes = pl.ds(0, DA) if half == "a" else pl.ds(DA, FFD - DA)
        return dt.at[zz, yy, cc, :, lanes]

    def stream(m, view, send_sem, recv_sem, ready):
        slots = {}

        def slot(key):
            return slots.setdefault(key, len(slots))

        def send(key, zz, yy, to):
            i = slot(key)
            ref = view(key[0], zz, yy, c)
            begin(remote(ref, ref, send_sem.at[i], recv_sem.at[i], to))

        def recv(key, zz, yy, cc):
            i = slot(key)
            ref = view(key[0], zz, yy, cc)
            remote(ref, ref, send_sem.at[i], recv_sem.at[i], to_core).wait_recv()

        def start():
            ready()
            send("ay-1", z, y, to_yp)
            send("ay+1", z, y, to_ym)
            send("bz-1", z, y, to_zp)
            send("bz+1", z, y, to_zm)

        def a_back():
            recv("ay-1", z, yat(-1), c)
            send("ay-2", z, yat(-1), to_yp)

        def a_out():
            send("az-1", z, ALL, to_zp)
            send("az+1", z, ALL, to_zm)
            send("ad0", z, ALL, to_core)

        steps[m + "start"] = start
        steps[m + "ay-1"] = a_back
        steps[m + "ay+1"] = lambda: recv("ay+1", z, yat(1), c)
        steps[m + "ay-2"] = lambda: recv("ay-2", z, yat(-2), c)
        steps[m + "ao"] = a_out

        def along_z(kind, k, yy):
            recv(f"{kind}z{k:+d}", zat(k), yy, c)
            if -4 < k < 0:
                send(f"{kind}z{k - 1:+d}", zat(k), yy, to_zp)
            if 0 < k < 3:
                send(f"{kind}z{k + 1:+d}", zat(k), yy, to_zm)
            if kind == "a":
                send(f"ad{k}", zat(k), ALL, to_core)

        def b_out(k):
            send(f"by-1,{k}", zat(k), y, to_yp)
            send(f"by+1,{k}", zat(k), y, to_ym)

        def b_back(k):
            recv(f"by-1,{k}", zat(k), yat(-1), c)
            send(f"by-2,{k}", zat(k), yat(-1), to_yp)

        def b_last(k):
            recv(f"by-2,{k}", zat(k), yat(-2), c)
            send(f"bd{k}", zat(k), ALL, to_core)

        def partner(kind, k):
            recv(f"{kind}d{k}", (z - k * s + NZ) % NZ, ALL, 1 - c)

        for k in LABELS:
            if k:
                steps[m + f"az{k:+d}"] = lambda k=k: along_z("a", k, ALL)
                steps[m + f"bz{k:+d}"] = lambda k=k: along_z("b", k, y)
            steps[m + f"bo{k}"] = lambda k=k: b_out(k)
            steps[m + f"by-1,{k}"] = lambda k=k: b_back(k)
            steps[m + f"by+1,{k}"] = lambda k=k: recv(f"by+1,{k}", zat(k), yat(1), c)
            steps[m + f"by-2,{k}"] = lambda k=k: b_last(k)
            steps[m + f"ad{k}"] = lambda k=k: partner("a", k)
            steps[m + f"bd{k}"] = lambda k=k: partner("b", k)

    stream("g", gu_at, gs, gr, lambda: loaded(gu.at[:, z, y, c], 0))
    stream("d", dt_at, ds_, dr, lambda: loaded(dt.at[z, y, c], 4))

    qi = lax.broadcasted_iota(jnp.int32, (WINDOW, 2 * WINDOW), 0)
    ki = lax.broadcasted_iota(jnp.int32, (WINDOW, 2 * WINDOW), 1)
    rel = qi + WINDOW - ki
    bias[...] = jnp.where((rel >= 0) & (rel < WINDOW), 0.0, -1e30)
    low = lax.broadcasted_iota(jnp.int32, (WINDOW, WINDOW), 1) < HEAD
    low_b = low.astype(F32).astype(BF16)
    high_b = 1 - low_b

    def attend(b, first):
        rows = pl.ds(b * WINDOW, WINDOW)
        band = pl.ds(b * WINDOW, 2 * WINDOW)
        q = [qv[rows, t * WINDOW : (t + 1) * WINDOW] for t in range(2)]
        q = jnp.concatenate([q[0] * low_b, q[0] * high_b, q[1] * low_b, q[1] * high_b], axis=0)
        score = jnp.dot(q, kx[:, band], preferred_element_type=F32)
        off = bias[...]
        if first:
            off = jnp.where((ki < WINDOW) & (sp == 0), -1e30, off)
        weights = []
        for h in range(4):
            one = score[h * WINDOW : (h + 1) * WINDOW] * HEAD ** (-0.5) + off
            top = jnp.maximum(jnp.max(one, axis=-1, keepdims=True), sink_s[h])
            expd = jnp.exp(one - top)
            denom = jnp.sum(expd, axis=-1, keepdims=True) + jnp.exp(sink_s[h] - top)
            weights.append((expd * (1.0 / denom)).astype(BF16))
        weights = jnp.concatenate(weights, axis=0)
        o = lax.dot_general(weights, vx[:, band], NT, preferred_element_type=F32)
        for t in range(2):
            even = o[2 * t * WINDOW : (2 * t + 1) * WINDOW]
            odd = o[(2 * t + 1) * WINDOW : (2 * t + 2) * WINDOW]
            ao[rows, t * WINDOW : (t + 1) * WINDOW] = jnp.where(low, even, odd).astype(BF16)

    def halo_copy(i, buf):
        return remote(
            buf.at[:, pl.ds(ROWS, WINDOW)], buf.at[:, pl.ds(0, WINDOW)], hsem.at[i], hsem.at[2 + i], to_next
        )

    def halo():
        @pl.when(sp < nsp - 1)
        def _():
            for i, buf in enumerate((kx, vx)):
                halo_copy(i, buf).start()

    def attend_first():
        @pl.when(sp > 0)
        def _():
            for i, buf in enumerate((kx, vx)):
                halo_copy(i, buf).wait_recv()

        @pl.when(sp == 0)
        def _():
            for buf in (kx, vx):
                buf[:, :WINDOW] = jnp.zeros((2 * HEAD, WINDOW), BF16)

        attend(0, True)

    steps["halo"] = halo
    steps["at0"] = attend_first
    for b in range(1, 6):
        steps[f"at{b}"] = lambda b=b: attend(b, False)

    def exchange():
        for j in (1, 2, 3):
            to = (x + j) % NX
            mine = ao.at[pl.ds(pl.multiple_of(to * MINE, MINE), MINE)]
            begin(remote(mine, at.at[x], as_.at[j], ar.at[j], {"tp": to}))
        at[x] = ao[pl.ds(pl.multiple_of(x * MINE, MINE), MINE), :]

    def rows_copy(kind, j):
        return remote(
            xs.at[(0, 0, 1)[kind], pl.ds(48 * j, 48)], xs.at[(1, 2, 3)[kind], pl.ds(48 * j, 48)],
            xsend.at[4 * kind + j], xrecv.at[4 * kind + j], (to_xp, to_xm, to_xp)[kind],
        )

    def project():
        for j in (1, 2, 3):
            src = (x + NX - j) % NX
            remote(at.at[src], at.at[src], as_.at[j], ar.at[j], to_xp).wait_recv()
        loaded(wo, 5)
        loaded(res, 6)
        loaded(gain, 7)
        square = jnp.zeros((MINE, 1), F32)
        for n in range(8):
            proj = jnp.zeros((MINE, 256), F32)
            for i in range(NX):
                proj += jnp.dot(at[i], wo[n, 256 * i : 256 * (i + 1), :], preferred_element_type=F32)
            m = (res[n].astype(F32) + proj).astype(BF16)
            mix[n] = m
            mf = m.astype(F32)
            square += jnp.sum(mf * mf, axis=-1, keepdims=True)
        scale = lax.rsqrt(square * (1.0 / D) + 1e-06)
        for n in range(8):
            at_n = slice(256 * n, 256 * (n + 1))
            xs[0, :, at_n] = (mix[n].astype(F32) * scale * gain[:, at_n]).astype(BF16)
        for j in range(4):
            begin(rows_copy(0, j))
            begin(rows_copy(1, j))

    def pass_on(j):
        rows_copy(0, j).wait_recv()
        begin(rows_copy(2, j))

    steps["a2a"] = exchange
    steps["oproj"] = project
    for j in range(4):
        steps[f"xf{j}"] = lambda j=j: pass_on(j)
        steps[f"xm{j}"] = lambda j=j: rows_copy(1, j).wait_recv()
        steps[f"xa{j}"] = lambda j=j: rows_copy(2, j).wait_recv()

    def hidden(pair, n):
        rows = xs[2 * pair : 2 * pair + 2].reshape(2 * MINE, D)
        both = jnp.dot(rows, gu[n].reshape(D, 256), preferred_element_type=F32)
        gate, up = both[:, :128], both[:, 128:]
        h = (gate / (1.0 + jnp.exp(-gate)) * up).astype(BF16).reshape(2, MINE, 128)
        at_n = pl.ds(pl.multiple_of(n * 128, 128), 128)
        hid[2 * pair : 2 * pair + 2, :, at_n] = h

    def hidden_run(pair, lo, hi):
        pl.loop(lo + none, hi + none)(lambda n: hidden(pair, n))

    def partial(pair, n):
        rows = hid[2 * pair : 2 * pair + 2].reshape(2 * MINE, FFD)
        w = dt[zat(LABELS[n])].reshape(256, FFD)
        both = lax.dot_general(rows, w, NT, preferred_element_type=F32)
        return both[:MINE], both[MINE:]

    def sum_copy(kind, j):
        two = pl.ds(2 * j, 2)
        return remote(
            (sa, sm, sp_)[kind].at[two], (ra, rfp, rfm)[kind].at[two],
            rsend.at[4 * kind + j], rrecv.at[4 * kind + j], (to_xp, to_xm, to_xp)[kind],
        )

    def far_sums(j):
        for n in (2 * j, 2 * j + 1):
            near, far = partial(1, n)
            part[n] = near
            sa[n] = far.astype(BF16)
        begin(sum_copy(0, j))

    def near_sums(j):
        for n in (2 * j, 2 * j + 1):
            mine, back = partial(0, n)
            own[n] = mine + mix[zat(LABELS[n])].astype(F32)
            sm[n] = back.astype(BF16)
        begin(sum_copy(1, j))

    def add_on(j):
        sum_copy(0, j).wait_recv()
        for n in (2 * j, 2 * j + 1):
            sp_[n] = (part[n] + ra[n].astype(F32)).astype(BF16)
        begin(sum_copy(2, j))

    def out_copy(n):
        at_n = pl.ds(pl.multiple_of(zat(LABELS[n]) * 256, 256), 256)
        return pltpu.make_async_copy(outv.at[n], out_h.at[:, at_n], out_sem.at[n])

    def finish(j):
        sum_copy(1, j).wait_recv()
        sum_copy(2, j).wait_recv()
        for n in (2 * j, 2 * j + 1):
            outv[n] = (own[n] + rfp[n].astype(F32) + rfm[n].astype(F32)).astype(BF16)
            out_copy(n).start()

    for j in range(4):
        steps[f"pa{j}"] = lambda j=j: far_sums(j)
        steps[f"pm{j}"] = lambda j=j: near_sums(j)
        steps[f"sp{j}"] = lambda j=j: add_on(j)
        steps[f"fin{j}"] = lambda j=j: finish(j)

    loaded(qv, 3)
    loaded(kx.at[:, pl.ds(WINDOW, ROWS)], 1)
    loaded(vx.at[:, pl.ds(WINDOW, ROWS)], 2)
    for b in EARLY:
        attend(b, False)
    pl.semaphore_wait(barrier, len(peers))
    for name in ORDER:
        if name[0] == "h" and name[1] in "01":
            hidden_run(*(int(v) for v in name[1:].split(",")))
        else:
            steps[name]()
    @pl.when(sp < nsp - 1)
    def _():
        for i, buf in enumerate((kx, vx)):
            halo_copy(i, buf).wait_send()

    for copy in sent:
        copy.wait_send()
    for n in range(8):
        out_copy(n).wait()


def shards(residual, queries, keys, values, sinks, out_weight, norm_gain, gate, up, down):
    vmem = pltpu.VMEM
    dma = pltpu.SemaphoreType.DMA
    anyspec = pl.BlockSpec(memory_space=pl.ANY)
    smem = pl.BlockSpec(memory_space=pltpu.SMEM)
    return pl.pallas_call(
        kernel,
        out_shape=jax.ShapeDtypeStruct((MINE, D), BF16),
        in_specs=[anyspec] * 4 + [smem] + [anyspec] * 5,
        out_specs=anyspec,
        scratch_shapes=[
            vmem((11, NZ, NY, NC, 32, 256), BF16),
            vmem((NZ, NY, NC, 32, FFD), BF16),
            vmem((NX, MINE, D), BF16),
            vmem((NX, MINE, FFD), BF16),
            vmem((ROWS, 256), BF16),
            vmem((NX, MINE, 256), BF16),
            vmem((8, 1024, 256), BF16),
            vmem((8, MINE, 256), BF16),
            vmem((8, MINE, 256), BF16),
            vmem((ROWS, 256), BF16),
            vmem((2 * HEAD, ROWS + WINDOW), BF16),
            vmem((2 * HEAD, ROWS + WINDOW), BF16),
            vmem((1, D), F32),
            vmem((WINDOW, 2 * WINDOW), F32),
        ]
        + [vmem((8, MINE, 256), BF16)] * 6
        + [
            vmem((8, MINE, 256), F32),
            vmem((8, MINE, 256), F32),
            vmem((8, MINE, 256), BF16),
            dma((8,)),
            dma((8,)),
            dma((PER,)), dma((PER,)), dma((PER,)), dma((PER,)),
            dma((4,)), dma((4,)),
            dma((12,)), dma((12,)),
            dma((12,)), dma((12,)),
            dma((4,)),
        ],
        compiler_params=pltpu.CompilerParams(
            collective_id=0, has_side_effects=True, vmem_limit_bytes=62 * 1024 * 1024
        ),
    )(residual, queries, keys.T, values.T, sinks, out_weight, norm_gain.reshape(1, D), gate, up, down.T)


def solution(mesh):
    placed = (
        P(("sp", "tp"), None),
        P("sp", "tp"),
        P("sp", "tp"),
        P("sp", "tp"),
        P("tp"),
        P(),
        P(),
        P("sp", "tp"),
        P("sp", "tp"),
        P("tp", "sp"),
    )
    return jax.shard_map(
        shards, mesh=mesh, in_specs=placed, out_specs=P(("sp", "tp"), None), check_vma=False
    )
```

```python
import jax
import jax.numpy as jnp
from jax import lax
from jax.experimental import pallas as pl
from jax.experimental.pallas import tpu as pltpu
from jax.sharding import PartitionSpec as P

MESH = pl.DeviceIdType.MESH
BF16, F32 = jnp.bfloat16, jnp.float32
HEAD = 64
WINDOW = 128
NZ, NY, NC, NX = 8, 4, 2, 4
ROWS = 768
MINE = 192
D, FFD = 2048, 1408
TILES = ((0, 5, 2), (5, 11, 7))
DA = 640
NT = (((1,), (1,)), ((), ()))
LABELS = (0, -1, 1, -2, 2, -3, 3, -4)
PER = 57

G, Q, R, W = 0, 1, 2, 3
START, AY, AO, AZ, BZ, BO, BY, AD, BD = range(9)
HALO, EX, AT, PROJ, XN, XF, XM, XA, HID, PA, PN, SUM, FIN = range(20, 33)
ORDER = (
    (G, START), (HALO,), (G, BO, 0), (AT, 4), (EX, 2), (EX, 1), (Q, START), (Q, BO, 0), (AT, 5), (EX, 3), (AT, 0),
    (EX, 0), (G, AY, -1), (G, AY, 1), (G, BZ, 1), (G, BO, 1), (G, BZ, -1), (G, BO, -1), (G, BY, 1, 0), (Q, BZ, -1),
    (Q, BO, -1), (Q, AY, -1), (Q, BZ, 1), (Q, BO, 1), (Q, AY, 1), (Q, BY, 1, 0), (G, BY, -1, 0), (G, BZ, -2),
    (G, BO, -2), (G, AY, -2), (G, AO), (G, BY, 1, 1), (PROJ,), (Q, BZ, -2), (XN, 1), (Q, BZ, 2), (Q, BO, -2),
    (Q, BO, 2), (G, AD, 0), (G, BY, 1, -1), (G, BY, -1, 1), (G, BY, -1, -1), (Q, BY, 1, -1), (G, BZ, -3),
    (Q, BY, 1, 1), (Q, AY, -2), (Q, AO), (G, BY, 1, -2), (G, AZ, 1), (Q, BY, -1, 1), (Q, AD, 0), (G, AZ, -1),
    (Q, BY, 1, -2), (G, BY, -2, 0), (G, AD, 1), (Q, BZ, 3), (Q, BO, 3), (G, AD, -1), (Q, BZ, -3), (Q, BO, -3),
    (G, BZ, 2), (XN, 2), (Q, BY, 1, 2), (G, BD, 0), (XM, 1), (Q, BY, -1, -2), (G, BZ, -4), (G, BO, -4), (G, BO, -3),
    (Q, BY, -1, 2), (Q, AZ, 1), (XF, 1), (Q, BY, 1, 3), (Q, AD, 1), (Q, AZ, -1), (W, START), (Q, BY, 1, -3),
    (G, AZ, 2), (Q, AD, -1), (Q, BY, -2, 1), (G, BY, 1, -4), (G, BZ, 3), (G, BO, 3), (G, AD, 2), (G, BY, 1, -3),
    (Q, BY, -1, 3), (G, AZ, -2), (Q, BD, 1), (XM, 2), (XF, 2), (W, AY, 1), (Q, BY, -1, -3), (Q, BZ, -4),
    (Q, BO, -4), (G, AD, -2), (Q, BY, -2, -2), (Q, AZ, 2), (G, BY, -2, 1), (XF, 3), (G, BY, 1, 3), (G, BY, -1, -2),
    (Q, BY, -1, -1), (Q, BD, -2), (G, BO, 2), (Q, AD, 2), (G, BD, 1), (Q, AZ, -2), (XA, 1), (XF, 0), (W, AY, -1),
    (W, BZ, -1), (Q, BY, 1, -4), (Q, AD, -2), (G, BY, -1, 3), (G, AZ, 3), (XA, 2), (G, BY, 1, 2), (G, AD, 3),
    (Q, BY, -2, -3), (G, AZ, -3), (Q, BY, -1, 0), (Q, BY, -1, -4), (W, BO, 0), (W, BO, -1), (Q, AZ, 3), (XA, 3),
    (G, BY, -2, -2), (Q, BD, -3), (G, AD, -3), (XN, 0), (Q, BY, -2, -1), (W, BZ, 1), (Q, AZ, -3), (W, BO, 1),
    (G, BY, -1, -4), (Q, AD, 3), (G, BY, -1, 2), (G, BD, -2), (W, AY, -2), (W, AO), (Q, BY, -2, 3), (XA, 0),
    (Q, BD, -1), (G, BY, -2, 3), (Q, AD, -3), (Q, BY, -2, 2), (G, AZ, -4), (W, BY, 1, 0), (W, AD, 0), (Q, BD, 3),
    (Q, BY, -2, 0), (G, BY, -1, -3), (G, BD, 3), (W, BY, 1, -1), (W, BZ, 2), (Q, BD, 2), (W, BO, 2), (G, AD, -4),
    (HID, 2, 2, 0, 1), (Q, BY, -2, -4), (W, BY, 1, 1), (HID, 2, 2, 1, 2), (W, BY, -1, 0), (Q, BD, 0),
    (G, BY, -2, -1), (XM, 0), (Q, AZ, -4), (W, BY, -1, -1), (W, BY, -1, 1), (Q, BD, -4), (HID, 2, 2, 9, 11),
    (Q, AD, -4), (W, AZ, 1), (G, BY, -2, -4), (W, BY, 1, 2), (G, BD, -1), (HID, 2, 2, 6, 7), (W, BZ, -2),
    (W, BZ, 3), (G, BY, -2, -3), (W, BO, -2), (G, BY, -2, 2), (W, BO, 3), (HID, 2, 2, 5, 6), (W, AZ, -1),
    (W, AD, 1), (G, BD, -4), (W, BY, -1, 2), (HID, 2, 2, 7, 8), (G, BD, -3), (W, BY, -2, -1), (W, BY, -2, 0),
    (HID, 2, 2, 8, 9), (G, BD, 2), (HID, 2, 2, 2, 3), (W, AD, -1), (W, BY, -2, 1), (HID, 2, 2, 3, 4), (W, BZ, -3),
    (W, BD, -1), (W, BY, -1, -2), (W, BD, 0), (W, BO, -3), (W, BY, 1, -2), (XN, 3), (HID, 2, 2, 4, 5), (W, AZ, 2),
    (W, BD, 1), (PA, 0), (W, BY, 1, 3), (W, BY, -1, 3), (W, BY, -2, 2), (W, AZ, -2), (W, AD, 2), (W, BZ, -4),
    (W, BO, -4), (W, BD, 2), (W, BY, -2, -2), (PA, 1), (W, BY, -1, -3), (W, BY, 1, -3), (W, AD, -2), (W, BY, -2, 3),
    (W, BD, -2), (XM, 3), (HID, 0, 2, 1, 2), (W, AZ, 3), (HID, 0, 2, 0, 1), (W, BY, 1, -4), (W, BY, -1, -4),
    (W, BD, 3), (HID, 0, 2, 10, 11), (W, BY, -2, -3), (W, AZ, -3), (W, AD, 3), (PA, 2), (HID, 0, 2, 3, 4),
    (W, BD, -3), (HID, 0, 2, 7, 8), (W, AD, -3), (HID, 0, 2, 9, 10), (W, BY, -2, -4), (HID, 0, 2, 5, 6),
    (HID, 0, 2, 2, 3), (HID, 0, 2, 8, 9), (W, AZ, -4), (W, BD, -4), (HID, 0, 2, 4, 5), (HID, 0, 2, 6, 7), (PN, 0),
    (W, AD, -4), (PA, 3), (SUM, 0), (PN, 1), (SUM, 1), (PN, 2), (SUM, 2), (PN, 3), (SUM, 3), (FIN, 0), (FIN, 1),
    (FIN, 2), (FIN, 3),
)


def kernel(
    res_h, q_h, k_h, v_h, sink_s, wo_h, gain_h, g_h, u_h, d_h, out_h,
    gu, dt, xs, hid, ao, at, wo, res, mix, qv, kx, vx, gain, bias,
    sa, sm, sp_, ra, rfm, rfp, own, part, outv,
    load_sem, out_sem, gus, gur, ds_, dr, as_, ar, xsend, xrecv, rsend, rrecv, hsem,
):
    sp = lax.axis_index("sp")
    x = lax.axis_index("tp")
    z, y, c = sp // (NY * NC), (sp // NC) % NY, sp % NC
    s = 1 - 2 * c

    def spidx(zz, yy, cc):
        return (zz * NY + yy) * NC + cc

    def zat(k):
        return (z + k * s + NZ) % NZ

    def yat(k):
        return (y + k * s + NY) % NY

    def xat(k):
        return (x + k * s + NX) % NX

    to_yp = {"sp": spidx(z, yat(1), c)}
    to_ym = {"sp": spidx(z, yat(-1), c)}
    to_zp = {"sp": spidx(zat(1), y, c)}
    to_zm = {"sp": spidx(zat(-1), y, c)}
    to_core = {"sp": spidx(z, y, 1 - c)}
    to_xp = {"tp": xat(1)}
    to_xm = {"tp": xat(-1)}
    nsp = NZ * NY * NC
    none = sp // nsp
    to_next = {"sp": (sp + 1) % nsp}
    to_prev = {"sp": (sp + nsp - 1) % nsp}

    barrier = pltpu.get_barrier_semaphore()
    peers = [to_yp, to_ym, to_zp, to_zm, to_core, to_next, to_prev]
    peers += [{"tp": (x + j) % NX} for j in (1, 2, 3)]
    for peer in peers:
        pl.semaphore_signal(barrier, inc=1, device_id=peer, device_id_type=MESH)

    def load(src, dst, i):
        pltpu.make_async_copy(src, dst, load_sem.at[i]).start()

    def loaded(dst, i):
        pltpu.make_async_copy(dst, dst, load_sem.at[i]).wait()

    for n in range(11):
        load(g_h.at[:, pl.ds(128 * n, 128)], gu.at[n, z, y, c, :, pl.ds(0, 128)], 0)
        load(u_h.at[:, pl.ds(128 * n, 128)], gu.at[n, z, y, c, :, pl.ds(128, 128)], 0)
    load(q_h, qv, 3)
    for half in range(2):
        load(k_h, kx.at[pl.ds(half * HEAD, HEAD), pl.ds(WINDOW, ROWS)], 1)
        load(v_h, vx.at[pl.ds(half * HEAD, HEAD), pl.ds(WINDOW, ROWS)], 2)
    load(d_h, dt.at[z, y, c], 4)
    for n in range(8):
        load(wo_h.at[:, pl.ds(256 * n, 256)], wo.at[n], 5)
        load(res_h.at[:, pl.ds(256 * n, 256)], res.at[n], 6)
    load(gain_h, gain, 7)

    def remote(src, dst, send, recv, to):
        return pltpu.make_async_remote_copy(
            src_ref=src, dst_ref=dst, send_sem=send, recv_sem=recv, device_id=to, device_id_type=MESH
        )

    steps = {}
    sent = []

    def begin(copy):
        copy.start()
        sent.append(copy)

    ALL = slice(None)

    def gu_at(first, split, last):
        def at(half, zz, yy, cc):
            tiles = pl.ds(first, split - first) if half == 0 else pl.ds(split, last - split)
            return gu.at[tiles, zz, yy, cc]

        return at

    def dt_at(half, zz, yy, cc):
        lanes = pl.ds(0, DA) if half == 0 else pl.ds(DA, FFD - DA)
        return dt.at[zz, yy, cc, :, lanes]

    def stream(m, view, send_sem, recv_sem, ready):
        slots = {}

        def slot(key):
            return slots.setdefault(key, len(slots))

        def send(key, zz, yy, to):
            i = slot(key)
            ref = view(key[0], zz, yy, c)
            begin(remote(ref, ref, send_sem.at[i], recv_sem.at[i], to))

        def recv(key, zz, yy, cc):
            i = slot(key)
            ref = view(key[0], zz, yy, cc)
            remote(ref, ref, send_sem.at[i], recv_sem.at[i], to_core).wait_recv()

        def start():
            ready()
            send((0, AY, -1), z, y, to_yp)
            send((0, AY, 1), z, y, to_ym)
            send((1, BZ, -1), z, y, to_zp)
            send((1, BZ, 1), z, y, to_zm)

        def a_y(k):
            recv((0, AY, k), z, yat(k), c)
            if k == -1:
                send((0, AY, -2), z, yat(-1), to_yp)

        def a_out():
            send((0, AZ, -1), z, ALL, to_zp)
            send((0, AZ, 1), z, ALL, to_zm)
            send((0, AD, 0), z, ALL, to_core)

        def along_z(half, kind, k, yy):
            recv((half, kind, k), zat(k), yy, c)
            if -4 < k < 0:
                send((half, kind, k - 1), zat(k), yy, to_zp)
            if 0 < k < 3:
                send((half, kind, k + 1), zat(k), yy, to_zm)
            if half == 0:
                send((0, AD, k), zat(k), ALL, to_core)

        def b_out(k):
            send((1, BY, -1, k), zat(k), y, to_yp)
            send((1, BY, 1, k), zat(k), y, to_ym)

        def b_y(u, k):
            recv((1, BY, u, k), zat(k), yat(u), c)
            if u == -1:
                send((1, BY, -2, k), zat(k), yat(-1), to_yp)
            if u == -2:
                send((1, BD, k), zat(k), ALL, to_core)

        def partner(half, kind, k):
            recv((half, kind, k), (z - k * s + NZ) % NZ, ALL, 1 - c)

        steps[(m, START)] = start
        steps[(m, AO)] = a_out
        steps[(m, AY)] = a_y
        steps[(m, AZ)] = lambda k: along_z(0, AZ, k, ALL)
        steps[(m, BZ)] = lambda k: along_z(1, BZ, k, y)
        steps[(m, BO)] = b_out
        steps[(m, BY)] = b_y
        steps[(m, AD)] = lambda k: partner(0, AD, k)
        steps[(m, BD)] = lambda k: partner(1, BD, k)

    for i, (m, (first, last, split)) in enumerate(zip((G, Q, R), TILES)):
        ready = (lambda: None) if i else (lambda: loaded(gu.at[:, z, y, c], 0))
        stream(m, gu_at(first, split, last), gus.at[i], gur.at[i], ready)
    stream(W, dt_at, ds_, dr, lambda: loaded(dt.at[z, y, c], 4))

    qi = lax.broadcasted_iota(jnp.int32, (WINDOW, 2 * WINDOW), 0)
    ki = lax.broadcasted_iota(jnp.int32, (WINDOW, 2 * WINDOW), 1)
    rel = qi + WINDOW - ki
    bias[...] = jnp.where((rel >= 0) & (rel < WINDOW), 0.0, -1e30)
    low = lax.broadcasted_iota(jnp.int32, (WINDOW, WINDOW), 1) < HEAD
    low_b = low.astype(F32).astype(BF16)
    high_b = 1 - low_b

    def attend(b, first):
        rows = pl.ds(b * WINDOW, WINDOW)
        band = pl.ds(b * WINDOW, 2 * WINDOW)
        q = [qv[rows, t * WINDOW : (t + 1) * WINDOW] for t in range(2)]
        q = jnp.concatenate([q[0] * low_b, q[0] * high_b, q[1] * low_b, q[1] * high_b], axis=0)
        score = jnp.dot(q, kx[:, band], preferred_element_type=F32)
        off = bias[...]
        if first:
            off = jnp.where((ki < WINDOW) & (sp == 0), -1e30, off)
        weights = []
        for h in range(4):
            one = score[h * WINDOW : (h + 1) * WINDOW] * HEAD ** (-0.5) + off
            top = jnp.maximum(jnp.max(one, axis=-1, keepdims=True), sink_s[h])
            expd = jnp.exp(one - top)
            denom = jnp.sum(expd, axis=-1, keepdims=True) + jnp.exp(sink_s[h] - top)
            weights.append((expd * (1.0 / denom)).astype(BF16))
        weights = jnp.concatenate(weights, axis=0)
        o = lax.dot_general(weights, vx[:, band], NT, preferred_element_type=F32)
        for t in range(2):
            even = o[2 * t * WINDOW : (2 * t + 1) * WINDOW]
            odd = o[(2 * t + 1) * WINDOW : (2 * t + 2) * WINDOW]
            ao[rows, t * WINDOW : (t + 1) * WINDOW] = jnp.where(low, even, odd).astype(BF16)

    def halo_copy(i, buf):
        return remote(
            buf.at[:, pl.ds(ROWS, WINDOW)], buf.at[:, pl.ds(0, WINDOW)], hsem.at[i], hsem.at[2 + i], to_next
        )

    def halo():
        @pl.when(sp < nsp - 1)
        def _():
            for i, buf in enumerate((kx, vx)):
                halo_copy(i, buf).start()

    def attend_first():
        @pl.when(sp > 0)
        def _():
            for i, buf in enumerate((kx, vx)):
                halo_copy(i, buf).wait_recv()

        @pl.when(sp == 0)
        def _():
            for buf in (kx, vx):
                buf[:, :WINDOW] = jnp.zeros((2 * HEAD, WINDOW), BF16)

        attend(0, True)

    steps[HALO] = halo
    steps[AT] = lambda b: attend(b, False) if b else attend_first()

    def exchange_copy(to):
        return remote(ao.at[pl.ds(to * MINE, MINE)], at.at[x], as_.at[to], ar.at[x], {"tp": to})

    def exchange(to):
        @pl.when(x != to)
        def _():
            exchange_copy(to).start()

    def exchanged(src):
        @pl.when(x != src)
        def _():
            remote(at.at[src], at.at[src], as_.at[src], ar.at[src], to_xp).wait_recv()

    def rows_copy(kind, j):
        return remote(
            xs.at[(0, 0, 2)[kind], pl.ds(48 * j, 48)], xs.at[(2, 1, 3)[kind], pl.ds(48 * j, 48)],
            xsend.at[4 * kind + j], xrecv.at[4 * kind + j], (to_xp, to_xm, to_xp)[kind],
        )

    def project():
        at[x] = ao[pl.ds(pl.multiple_of(x * MINE, MINE), MINE), :]
        for j in range(NX):
            exchanged(j)
        loaded(wo, 5)
        loaded(res, 6)
        loaded(gain, 7)
        square = jnp.zeros((MINE, 1), F32)
        for n in range(8):
            proj = jnp.zeros((MINE, 256), F32)
            for i in range(NX):
                proj += jnp.dot(at[i], wo[n, 256 * i : 256 * (i + 1), :], preferred_element_type=F32)
            m = (res[n].astype(F32) + proj).astype(BF16)
            mix[n] = m
            mf = m.astype(F32)
            square += jnp.sum(mf * mf, axis=-1, keepdims=True)
        scale = lax.rsqrt(square * (1.0 / D) + 1e-06)
        for n in range(8):
            at_n = slice(256 * n, 256 * (n + 1))
            xs[0, :, at_n] = (mix[n].astype(F32) * scale * gain[:, at_n]).astype(BF16)
        for j in range(4):
            begin(rows_copy(0, j))

    def pass_on(j):
        rows_copy(0, j).wait_recv()
        begin(rows_copy(2, j))

    steps[EX] = exchange
    steps[PROJ] = project
    steps[XF] = pass_on
    steps[XN] = lambda j: begin(rows_copy(1, j))
    steps[XM] = lambda j: rows_copy(1, j).wait_recv()
    steps[XA] = lambda j: rows_copy(2, j).wait_recv()

    def hidden(lo, count, first, last):
        @pl.loop(first + none, last + none)
        def _(n):
            rows = xs[lo : lo + count].reshape(count * MINE, D)
            both = jnp.dot(rows, gu[n].reshape(D, 256), preferred_element_type=F32)
            gate, up = both[:, :128], both[:, 128:]
            h = (gate / (1.0 + jnp.exp(-gate)) * up).astype(BF16)
            hid[lo : lo + count, :, pl.ds(pl.multiple_of(n * 128, 128), 128)] = h.reshape(count, MINE, 128)

    steps[HID] = hidden

    def partial(lo, count, n):
        rows = hid[lo : lo + count].reshape(count * MINE, FFD)
        w = dt[zat(LABELS[n])].reshape(256, FFD)
        both = lax.dot_general(rows, w, NT, preferred_element_type=F32)
        return both[:MINE], both[MINE:]

    def sum_copy(kind, j):
        two = pl.ds(2 * j, 2)
        return remote(
            (sa, sm, sp_)[kind].at[two], (ra, rfp, rfm)[kind].at[two],
            rsend.at[4 * kind + j], rrecv.at[4 * kind + j], (to_xp, to_xm, to_xp)[kind],
        )

    def sums_out(j):
        for n in (2 * j, 2 * j + 1):
            back, far = partial(2, 2, n)
            sa[n] = far.astype(BF16)
            sm[n] = back.astype(BF16)
        begin(sum_copy(0, j))
        begin(sum_copy(1, j))

    def sums_kept(j):
        for n in (2 * j, 2 * j + 1):
            mine, ahead = partial(0, 2, n)
            own[n] = mine + mix[zat(LABELS[n])].astype(F32)
            part[n] = ahead

    def add_on(j):
        sum_copy(0, j).wait_recv()
        for n in (2 * j, 2 * j + 1):
            sp_[n] = (part[n] + ra[n].astype(F32)).astype(BF16)
        begin(sum_copy(2, j))

    def out_copy(n):
        at_n = pl.ds(pl.multiple_of(zat(LABELS[n]) * 256, 256), 256)
        return pltpu.make_async_copy(outv.at[n], out_h.at[:, at_n], out_sem.at[n])

    def finish(j):
        sum_copy(1, j).wait_recv()
        sum_copy(2, j).wait_recv()
        for n in (2 * j, 2 * j + 1):
            outv[n] = (own[n] + rfp[n].astype(F32) + rfm[n].astype(F32)).astype(BF16)
            out_copy(n).start()

    steps[PA] = sums_out
    steps[PN] = sums_kept
    steps[SUM] = add_on
    steps[FIN] = finish

    loaded(qv, 3)
    loaded(kx.at[:, pl.ds(WINDOW, ROWS)], 1)
    loaded(vx.at[:, pl.ds(WINDOW, ROWS)], 2)
    for b in (1, 2, 3):
        attend(b, False)
    pl.semaphore_wait(barrier, len(peers))
    for name in ORDER:
        if name[0] <= W:
            steps[name[:2]](*name[2:])
        else:
            steps[name[0]](*name[1:])
    @pl.when(sp < nsp - 1)
    def _():
        for i, buf in enumerate((kx, vx)):
            halo_copy(i, buf).wait_send()

    for to in range(NX):

        @pl.when(x != to)
        def _(to=to):
            exchange_copy(to).wait_send()

    for copy in sent:
        copy.wait_send()
    for n in range(8):
        out_copy(n).wait()


def shards(residual, queries, keys, values, sinks, out_weight, norm_gain, gate, up, down):
    vmem = pltpu.VMEM
    dma = pltpu.SemaphoreType.DMA
    anyspec = pl.BlockSpec(memory_space=pl.ANY)
    smem = pl.BlockSpec(memory_space=pltpu.SMEM)
    return pl.pallas_call(
        kernel,
        out_shape=jax.ShapeDtypeStruct((MINE, D), BF16),
        in_specs=[anyspec] * 4 + [smem] + [anyspec] * 5,
        out_specs=anyspec,
        scratch_shapes=[
            vmem((11, NZ, NY, NC, 32, 256), BF16),
            vmem((NZ, NY, NC, 32, FFD), BF16),
            vmem((NX, MINE, D), BF16),
            vmem((NX, MINE, FFD), BF16),
            vmem((ROWS, 256), BF16),
            vmem((NX, MINE, 256), BF16),
            vmem((8, 1024, 256), BF16),
            vmem((8, MINE, 256), BF16),
            vmem((8, MINE, 256), BF16),
            vmem((ROWS, 256), BF16),
            vmem((2 * HEAD, ROWS + WINDOW), BF16),
            vmem((2 * HEAD, ROWS + WINDOW), BF16),
            vmem((1, D), F32),
            vmem((WINDOW, 2 * WINDOW), F32),
        ]
        + [vmem((8, MINE, 256), BF16)] * 6
        + [
            vmem((8, MINE, 256), F32),
            vmem((8, MINE, 256), F32),
            vmem((8, MINE, 256), BF16),
            dma((8,)),
            dma((8,)),
            dma((len(TILES), PER)), dma((len(TILES), PER)), dma((PER,)), dma((PER,)),
            dma((4,)), dma((4,)),
            dma((12,)), dma((12,)),
            dma((12,)), dma((12,)),
            dma((4,)),
        ],
        compiler_params=pltpu.CompilerParams(
            collective_id=0, has_side_effects=True, vmem_limit_bytes=62 * 1024 * 1024
        ),
    )(residual, queries, keys.T, values.T, sinks, out_weight, norm_gain.reshape(1, D), gate, up, down.T)


def solution(mesh):
    placed = (
        P(("sp", "tp"), None),
        P("sp", "tp"),
        P("sp", "tp"),
        P("sp", "tp"),
        P("tp"),
        P(),
        P(),
        P("sp", "tp"),
        P("sp", "tp"),
        P("tp", "sp"),
    )
    return jax.shard_map(
        shards, mesh=mesh, in_specs=placed, out_specs=P(("sp", "tp"), None), check_vma=False
    )
```

```python
import jax
import jax.numpy as jnp
from jax import lax
from jax.experimental import pallas as pl
from jax.experimental.pallas import tpu as pltpu
from jax.sharding import PartitionSpec as P

MESH = pl.DeviceIdType.MESH
BF16, F32 = jnp.bfloat16, jnp.float32
HEAD = 64
WINDOW = 128
NZ, NY, NC, NX = 8, 4, 2, 4
ROWS = 768
MINE = 192
D, FFD = 2048, 1408
TILES = ((0, 11, 4),)
DA = 512
NT = (((1,), (1,)), ((), ()))
LABELS = (0, -1, 1, -2, 2, -3, 3, -4)
PER = 57

G, Q, R, W = 0, 1, 2, 3
START, AY, AO, AZ, BZ, BO, BY, AD, BD = range(9)
HALO, EX, AT, PROJ, XN, XF, XM, XA, HID, PA, PN, SUM, FIN = range(20, 33)
ORDER = (
    (G, START), (HALO,), (G, BO, 0), (AT, 4), (AT, 1), (AT, 3), (EX, 2), (AT, 2), (AT, 0), (EX, 0), (AT, 5),
    (G, AY, -1), (EX, 3), (EX, 1), (G, BZ, -1), (G, BO, -1), (G, BZ, 1), (G, BO, 1), (G, BY, -1, 0), (G, AY, -2),
    (G, AY, 1), (G, AO), (PROJ,), (XN, 2), (G, BY, -1, -1), (G, BZ, 2), (G, BO, 2), (XN, 0), (G, BZ, -2),
    (G, BO, -2), (G, BY, -1, 1), (G, BY, 1, 0), (G, BY, -2, 0), (G, AZ, -1), (G, AZ, 1), (W, START), (G, BY, 1, -1),
    (G, BY, -2, -1), (XF, 0), (G, BZ, -3), (G, BO, -3), (G, BZ, 3), (G, BO, 3), (G, BY, -1, 2), (XN, 1),
    (G, BY, -1, -2), (XF, 1), (G, BY, 1, 1), (G, BY, -2, 1), (W, AY, -1), (G, AZ, -2), (G, AZ, 2), (XF, 2),
    (G, BY, -1, -3), (G, BZ, -4), (G, BO, -4), (G, BY, -1, 3), (W, BO, 0), (XF, 3), (XN, 3), (W, BZ, -1),
    (W, BO, -1), (G, BY, 1, -2), (G, BY, -2, -2), (W, AY, -2), (W, AY, 1), (W, AO), (W, BZ, 1), (W, BO, 1),
    (G, AZ, -3), (G, AZ, 3), (G, BY, 1, -3), (G, BY, -2, -3), (W, BZ, -2), (G, BY, 1, 2), (G, BY, -2, 2),
    (G, BY, -1, -4), (W, AZ, -1), (W, AZ, 1), (G, BY, 1, 3), (G, BY, -2, 3), (W, BZ, 2), (W, BO, 2), (W, BY, -1, 0),
    (W, BY, -1, -1), (W, BY, -1, 1), (G, BY, 1, -4), (G, BY, -2, -4), (G, AZ, -4), (W, BY, -1, 2), (W, BO, -2),
    (W, BZ, -3), (W, BO, -3), (W, AZ, 2), (G, BD, 0), (G, BD, -1), (G, BD, 1), (XA, 0), (G, BD, -2), (XA, 1),
    (G, BD, -3), (G, BD, 2), (XA, 2), (XA, 3), (G, BD, 3), (G, BD, -4), (HID, 2, 2, 8, 3), (W, BY, 1, -1),
    (W, BY, -2, -1), (W, BZ, 3), (W, BO, 3), (W, BY, 1, 1), (W, BY, -2, 1), (W, BY, 1, 0), (W, BY, -2, 0),
    (G, AD, 0), (G, AD, -1), (G, AD, 1), (G, AD, -2), (G, AD, 2), (G, AD, -3), (G, AD, 3), (G, AD, -4),
    (HID, 2, 2, 2, 2), (HID, 2, 2, 0, 2), (W, BZ, -4), (W, BY, 1, 2), (W, BY, -2, 2), (W, BO, -4),
    (HID, 2, 2, 4, 2), (W, BY, -1, -2), (HID, 2, 2, 6, 2), (W, BY, -1, -3), (W, AD, 0), (W, AD, 1), (W, BD, 1),
    (W, BD, 0), (PA, 0), (W, BY, -1, 3), (W, AZ, -2), (W, AZ, 3), (XM, 2), (XM, 0), (XM, 1), (XM, 3),
    (HID, 0, 2, 4, 2), (W, BY, -1, -4), (W, BY, 1, -2), (W, BY, -2, -2), (W, AD, -1), (W, AD, 2), (W, BD, -1),
    (W, BD, 2), (PA, 1), (HID, 0, 2, 2, 2), (W, BY, 1, -3), (W, BY, -2, -3), (W, BY, 1, 3), (W, BY, -2, 3),
    (HID, 0, 2, 0, 2), (W, AZ, -3), (W, BY, 1, -4), (W, BY, -2, -4), (HID, 0, 2, 6, 2), (W, AD, -2), (W, AD, 3),
    (W, BD, -2), (W, BD, 3), (PA, 2), (HID, 0, 2, 8, 3), (PN, 2), (W, AZ, -4), (PN, 0), (SUM, 0), (PN, 1),
    (W, AD, -3), (W, BD, -4), (W, BD, -3), (W, AD, -4), (PA, 3), (SUM, 1), (PN, 3), (SUM, 2), (FIN, 0), (SUM, 3),
    (FIN, 1), (FIN, 2), (FIN, 3),
)


def kernel(
    res_h, q_h, k_h, v_h, sink_s, wo_h, gain_h, g_h, u_h, d_h, out_h,
    gu, dt, xs, hid, ao, at, wo, res, mix, qv, kx, vx, gain, bias,
    sa, sm, sp_, ra, rfm, rfp, own, part, outv,
    load_sem, out_sem, gus, gur, ds_, dr, as_, ar, xsend, xrecv, rsend, rrecv, hsem,
):
    sp = lax.axis_index("sp")
    x = lax.axis_index("tp")
    z, y, c = sp // (NY * NC), (sp // NC) % NY, sp % NC
    s = 1 - 2 * c

    def spidx(zz, yy, cc):
        return (zz * NY + yy) * NC + cc

    def zat(k):
        return (z + k * s + NZ) % NZ

    def yat(k):
        return (y + k * s + NY) % NY

    def xat(k):
        return (x + k * s + NX) % NX

    to_yp = {"sp": spidx(z, yat(1), c)}
    to_ym = {"sp": spidx(z, yat(-1), c)}
    to_zp = {"sp": spidx(zat(1), y, c)}
    to_zm = {"sp": spidx(zat(-1), y, c)}
    to_core = {"sp": spidx(z, y, 1 - c)}
    to_xp = {"tp": xat(1)}
    to_xm = {"tp": xat(-1)}
    nsp = NZ * NY * NC
    none = sp // nsp
    to_next = {"sp": (sp + 1) % nsp}
    to_prev = {"sp": (sp + nsp - 1) % nsp}

    barrier = pltpu.get_barrier_semaphore()
    peers = [to_yp, to_ym, to_zp, to_zm, to_core, to_next, to_prev]
    peers += [{"tp": (x + j) % NX} for j in (1, 2, 3)]
    for peer in peers:
        pl.semaphore_signal(barrier, inc=1, device_id=peer, device_id_type=MESH)

    def load(src, dst, i):
        pltpu.make_async_copy(src, dst, load_sem.at[i]).start()

    def loaded(dst, i):
        pltpu.make_async_copy(dst, dst, load_sem.at[i]).wait()

    for n in range(11):
        load(g_h.at[:, pl.ds(128 * n, 128)], gu.at[n, z, y, c, :, pl.ds(0, 128)], 0)
        load(u_h.at[:, pl.ds(128 * n, 128)], gu.at[n, z, y, c, :, pl.ds(128, 128)], 0)
    load(q_h, qv, 3)
    for half in range(2):
        load(k_h, kx.at[pl.ds(half * HEAD, HEAD), pl.ds(WINDOW, ROWS)], 1)
        load(v_h, vx.at[pl.ds(half * HEAD, HEAD), pl.ds(WINDOW, ROWS)], 2)
    load(d_h, dt.at[z, y, c], 4)
    for n in range(8):
        load(wo_h.at[:, pl.ds(256 * n, 256)], wo.at[n], 5)
        load(res_h.at[:, pl.ds(256 * n, 256)], res.at[n], 6)
    load(gain_h, gain, 7)

    def remote(src, dst, send, recv, to):
        return pltpu.make_async_remote_copy(
            src_ref=src, dst_ref=dst, send_sem=send, recv_sem=recv, device_id=to, device_id_type=MESH
        )

    steps = {}
    sent = []

    def begin(copy):
        copy.start()
        sent.append(copy)

    ALL = slice(None)

    def gu_at(first, split, last):
        def at(half, zz, yy, cc):
            tiles = pl.ds(first, split - first) if half == 0 else pl.ds(split, last - split)
            return gu.at[tiles, zz, yy, cc]

        return at

    def dt_at(half, zz, yy, cc):
        lanes = pl.ds(0, DA) if half == 0 else pl.ds(DA, FFD - DA)
        return dt.at[zz, yy, cc, :, lanes]

    def stream(m, view, send_sem, recv_sem, ready):
        slots = {}

        def slot(key):
            return slots.setdefault(key, len(slots))

        def send(key, zz, yy, to):
            i = slot(key)
            ref = view(key[0], zz, yy, c)
            begin(remote(ref, ref, send_sem.at[i], recv_sem.at[i], to))

        def recv(key, zz, yy, cc):
            i = slot(key)
            ref = view(key[0], zz, yy, cc)
            remote(ref, ref, send_sem.at[i], recv_sem.at[i], to_core).wait_recv()

        def start():
            ready()
            send((0, AY, -1), z, y, to_yp)
            send((0, AY, 1), z, y, to_ym)
            send((1, BZ, -1), z, y, to_zp)
            send((1, BZ, 1), z, y, to_zm)

        def a_y(k):
            recv((0, AY, k), z, yat(k), c)
            if k == -1:
                send((0, AY, -2), z, yat(-1), to_yp)

        def a_out():
            send((0, AZ, -1), z, ALL, to_zp)
            send((0, AZ, 1), z, ALL, to_zm)
            send((0, AD, 0), z, ALL, to_core)

        def along_z(half, kind, k, yy):
            recv((half, kind, k), zat(k), yy, c)
            if -4 < k < 0:
                send((half, kind, k - 1), zat(k), yy, to_zp)
            if 0 < k < 3:
                send((half, kind, k + 1), zat(k), yy, to_zm)
            if half == 0:
                send((0, AD, k), zat(k), ALL, to_core)

        def b_out(k):
            send((1, BY, -1, k), zat(k), y, to_yp)
            send((1, BY, 1, k), zat(k), y, to_ym)

        def b_y(u, k):
            recv((1, BY, u, k), zat(k), yat(u), c)
            if u == -1:
                send((1, BY, -2, k), zat(k), yat(-1), to_yp)
            if u == -2:
                send((1, BD, k), zat(k), ALL, to_core)

        def partner(half, kind, k):
            recv((half, kind, k), (z - k * s + NZ) % NZ, ALL, 1 - c)

        steps[(m, START)] = start
        steps[(m, AO)] = a_out
        steps[(m, AY)] = a_y
        steps[(m, AZ)] = lambda k: along_z(0, AZ, k, ALL)
        steps[(m, BZ)] = lambda k: along_z(1, BZ, k, y)
        steps[(m, BO)] = b_out
        steps[(m, BY)] = b_y
        steps[(m, AD)] = lambda k: partner(0, AD, k)
        steps[(m, BD)] = lambda k: partner(1, BD, k)

    for i, (m, (first, last, split)) in enumerate(zip((G, Q, R), TILES)):
        ready = (lambda: None) if i else (lambda: loaded(gu.at[:, z, y, c], 0))
        stream(m, gu_at(first, split, last), gus.at[i], gur.at[i], ready)
    stream(W, dt_at, ds_, dr, lambda: loaded(dt.at[z, y, c], 4))

    qi = lax.broadcasted_iota(jnp.int32, (WINDOW, 2 * WINDOW), 0)
    ki = lax.broadcasted_iota(jnp.int32, (WINDOW, 2 * WINDOW), 1)
    rel = qi + WINDOW - ki
    bias[...] = jnp.where((rel >= 0) & (rel < WINDOW), 0.0, -1e30)
    low = lax.broadcasted_iota(jnp.int32, (WINDOW, WINDOW), 1) < HEAD
    low_b = low.astype(F32).astype(BF16)
    high_b = 1 - low_b

    def attend(b, first):
        rows = pl.ds(b * WINDOW, WINDOW)
        band = pl.ds(b * WINDOW, 2 * WINDOW)
        q = [qv[rows, t * WINDOW : (t + 1) * WINDOW] for t in range(2)]
        q = jnp.concatenate([q[0] * low_b, q[0] * high_b, q[1] * low_b, q[1] * high_b], axis=0)
        score = jnp.dot(q, kx[:, band], preferred_element_type=F32)
        off = bias[...]
        if first:
            off = jnp.where((ki < WINDOW) & (sp == 0), -1e30, off)
        weights = []
        for h in range(4):
            one = score[h * WINDOW : (h + 1) * WINDOW] * HEAD ** (-0.5) + off
            top = jnp.maximum(jnp.max(one, axis=-1, keepdims=True), sink_s[h])
            expd = jnp.exp(one - top)
            denom = jnp.sum(expd, axis=-1, keepdims=True) + jnp.exp(sink_s[h] - top)
            weights.append((expd * (1.0 / denom)).astype(BF16))
        weights = jnp.concatenate(weights, axis=0)
        o = lax.dot_general(weights, vx[:, band], NT, preferred_element_type=F32)
        for t in range(2):
            even = o[2 * t * WINDOW : (2 * t + 1) * WINDOW]
            odd = o[(2 * t + 1) * WINDOW : (2 * t + 2) * WINDOW]
            ao[rows, t * WINDOW : (t + 1) * WINDOW] = jnp.where(low, even, odd).astype(BF16)

    def halo_copy(i, buf):
        return remote(
            buf.at[:, pl.ds(ROWS, WINDOW)], buf.at[:, pl.ds(0, WINDOW)], hsem.at[i], hsem.at[2 + i], to_next
        )

    def halo():
        loaded(qv, 3)
        loaded(kx.at[:, pl.ds(WINDOW, ROWS)], 1)
        loaded(vx.at[:, pl.ds(WINDOW, ROWS)], 2)

        @pl.when(sp < nsp - 1)
        def _():
            for i, buf in enumerate((kx, vx)):
                halo_copy(i, buf).start()

    def attend_first():
        @pl.when(sp > 0)
        def _():
            for i, buf in enumerate((kx, vx)):
                halo_copy(i, buf).wait_recv()

        @pl.when(sp == 0)
        def _():
            for buf in (kx, vx):
                buf[:, :WINDOW] = jnp.zeros((2 * HEAD, WINDOW), BF16)

        attend(0, True)

    steps[HALO] = halo
    steps[AT] = lambda b: attend(b, False) if b else attend_first()

    def exchange_copy(to):
        return remote(ao.at[pl.ds(to * MINE, MINE)], at.at[x], as_.at[to], ar.at[x], {"tp": to})

    def exchange(to):
        @pl.when(x != to)
        def _():
            exchange_copy(to).start()

    def exchanged(src):
        @pl.when(x != src)
        def _():
            remote(at.at[src], at.at[src], as_.at[src], ar.at[src], to_xp).wait_recv()

    def rows_copy(kind, j):
        return remote(
            xs.at[(0, 0, 2)[kind], pl.ds(48 * j, 48)], xs.at[(2, 1, 3)[kind], pl.ds(48 * j, 48)],
            xsend.at[4 * kind + j], xrecv.at[4 * kind + j], (to_xp, to_xm, to_xp)[kind],
        )

    def project():
        at[x] = ao[pl.ds(pl.multiple_of(x * MINE, MINE), MINE), :]
        for j in range(NX):
            exchanged(j)
        loaded(wo, 5)
        loaded(res, 6)
        loaded(gain, 7)
        square = jnp.zeros((MINE, 1), F32)
        for n in range(8):
            proj = jnp.zeros((MINE, 256), F32)
            for i in range(NX):
                proj += jnp.dot(at[i], wo[n, 256 * i : 256 * (i + 1), :], preferred_element_type=F32)
            m = (res[n].astype(F32) + proj).astype(BF16)
            mix[n] = m
            mf = m.astype(F32)
            square += jnp.sum(mf * mf, axis=-1, keepdims=True)
        scale = lax.rsqrt(square * (1.0 / D) + 1e-06)
        for n in range(8):
            at_n = slice(256 * n, 256 * (n + 1))
            xs[0, :, at_n] = (mix[n].astype(F32) * scale * gain[:, at_n]).astype(BF16)
        for j in range(4):
            begin(rows_copy(0, j))

    def pass_on(j):
        rows_copy(0, j).wait_recv()
        begin(rows_copy(2, j))

    steps[EX] = exchange
    steps[PROJ] = project
    steps[XF] = pass_on
    steps[XN] = lambda j: begin(rows_copy(1, j))
    steps[XM] = lambda j: rows_copy(1, j).wait_recv()
    steps[XA] = lambda j: rows_copy(2, j).wait_recv()

    def hidden(lo, count, first, width):
        @pl.loop(first + none, first + none + 1)
        def _(i):
            for u in range(width):
                n = i + u
                rows = xs[lo : lo + count].reshape(count * MINE, D)
                both = jnp.dot(rows, gu[n].reshape(D, 256), preferred_element_type=F32)
                gate, up = both[:, :128], both[:, 128:]
                h = (gate / (1.0 + jnp.exp(-gate)) * up).astype(BF16)
                hid[lo : lo + count, :, pl.ds(pl.multiple_of(n * 128, 128), 128)] = h.reshape(count, MINE, 128)

    steps[HID] = hidden

    def partial(lo, count, n):
        rows = hid[lo : lo + count].reshape(count * MINE, FFD)
        w = dt[zat(LABELS[n])].reshape(256, FFD)
        both = lax.dot_general(rows, w, NT, preferred_element_type=F32)
        return both[:MINE], both[MINE:]

    def sum_copy(kind, j):
        two = pl.ds(2 * j, 2)
        return remote(
            (sa, sm, sp_)[kind].at[two], (ra, rfp, rfm)[kind].at[two],
            rsend.at[4 * kind + j], rrecv.at[4 * kind + j], (to_xp, to_xm, to_xp)[kind],
        )

    def sums_out(j):
        for n in (2 * j, 2 * j + 1):
            back, far = partial(2, 2, n)
            sa[n] = far.astype(BF16)
            sm[n] = back.astype(BF16)
        begin(sum_copy(0, j))
        begin(sum_copy(1, j))

    def sums_kept(j):
        for n in (2 * j, 2 * j + 1):
            mine, ahead = partial(0, 2, n)
            own[n] = mine + mix[zat(LABELS[n])].astype(F32)
            part[n] = ahead

    def add_on(j):
        sum_copy(0, j).wait_recv()
        for n in (2 * j, 2 * j + 1):
            sp_[n] = (part[n] + ra[n].astype(F32)).astype(BF16)
        begin(sum_copy(2, j))

    def out_copy(n):
        at_n = pl.ds(pl.multiple_of(zat(LABELS[n]) * 256, 256), 256)
        return pltpu.make_async_copy(outv.at[n], out_h.at[:, at_n], out_sem.at[n])

    def finish(j):
        sum_copy(1, j).wait_recv()
        sum_copy(2, j).wait_recv()
        for n in (2 * j, 2 * j + 1):
            outv[n] = (own[n] + rfp[n].astype(F32) + rfm[n].astype(F32)).astype(BF16)
            out_copy(n).start()

    steps[PA] = sums_out
    steps[PN] = sums_kept
    steps[SUM] = add_on
    steps[FIN] = finish

    pl.semaphore_wait(barrier, len(peers))
    for name in ORDER:
        if name[0] <= W:
            steps[name[:2]](*name[2:])
        else:
            steps[name[0]](*name[1:])
    @pl.when(sp < nsp - 1)
    def _():
        for i, buf in enumerate((kx, vx)):
            halo_copy(i, buf).wait_send()

    for to in range(NX):

        @pl.when(x != to)
        def _(to=to):
            exchange_copy(to).wait_send()

    for copy in sent:
        copy.wait_send()
    for n in range(8):
        out_copy(n).wait()


def shards(residual, queries, keys, values, sinks, out_weight, norm_gain, gate, up, down):
    vmem = pltpu.VMEM
    dma = pltpu.SemaphoreType.DMA
    anyspec = pl.BlockSpec(memory_space=pl.ANY)
    smem = pl.BlockSpec(memory_space=pltpu.SMEM)
    return pl.pallas_call(
        kernel,
        out_shape=jax.ShapeDtypeStruct((MINE, D), BF16),
        in_specs=[anyspec] * 4 + [smem] + [anyspec] * 5,
        out_specs=anyspec,
        scratch_shapes=[
            vmem((11, NZ, NY, NC, 32, 256), BF16),
            vmem((NZ, NY, NC, 32, FFD), BF16),
            vmem((NX, MINE, D), BF16),
            vmem((NX, MINE, FFD), BF16),
            vmem((ROWS, 256), BF16),
            vmem((NX, MINE, 256), BF16),
            vmem((8, 1024, 256), BF16),
            vmem((8, MINE, 256), BF16),
            vmem((8, MINE, 256), BF16),
            vmem((ROWS, 256), BF16),
            vmem((2 * HEAD, ROWS + WINDOW), BF16),
            vmem((2 * HEAD, ROWS + WINDOW), BF16),
            vmem((1, D), F32),
            vmem((WINDOW, 2 * WINDOW), F32),
        ]
        + [vmem((8, MINE, 256), BF16)] * 6
        + [
            vmem((8, MINE, 256), F32),
            vmem((8, MINE, 256), F32),
            vmem((8, MINE, 256), BF16),
            dma((8,)),
            dma((8,)),
            dma((len(TILES), PER)), dma((len(TILES), PER)), dma((PER,)), dma((PER,)),
            dma((4,)), dma((4,)),
            dma((12,)), dma((12,)),
            dma((12,)), dma((12,)),
            dma((4,)),
        ],
        compiler_params=pltpu.CompilerParams(
            collective_id=0, has_side_effects=True, vmem_limit_bytes=62 * 1024 * 1024
        ),
    )(residual, queries, keys.T, values.T, sinks, out_weight, norm_gain.reshape(1, D), gate, up, down.T)


def solution(mesh):
    placed = (
        P(("sp", "tp"), None),
        P("sp", "tp"),
        P("sp", "tp"),
        P("sp", "tp"),
        P("tp"),
        P(),
        P(),
        P("sp", "tp"),
        P("sp", "tp"),
        P("tp", "sp"),
    )
    return jax.shard_map(
        shards, mesh=mesh, in_specs=placed, out_specs=P(("sp", "tp"), None), check_vma=False
    )
```
